32 devices in a mesh: ep: 16 (over z, y, x), tp: 2 (over core).
Axes of the slice: x: 2, y: 2, z: 4, core: 2. Of those that a mesh axis runs over, the one named last changes fastest.
Arguments:
- tokens: bfloat16 [4096, 2048], P(('ep', 'tp')), may hold values from -6 to 6
- norm_gain: float32 [2048], replicated, may hold values from 0.25 to 4
- routes: int32 [4096, 2], P(('ep', 'tp')), may hold values from 0 to 15, all different within a row; in each aligned block of 128 rows (0 to 127, 128 to 255, ...) at most 22 rows name the same one
- route_weights: float32 [4096, 2], P(('ep', 'tp')), may hold values from 0.1 to 1
- w_gate: bfloat16 [16, 2048, 1024], P('ep', None, 'tp'), may hold values from -0.125 to 0.125
- w_up: bfloat16 [16, 2048, 1024], P('ep', None, 'tp'), may hold values from -0.125 to 0.125
- w_down: bfloat16 [16, 1024, 2048], P('ep', 'tp'), may hold values from -0.1875 to 0.1875
- dense_in: bfloat16 [2048, 256], P('ep'), may hold values from -0.125 to 0.125
- dense_out: bfloat16 [2048, 256], P('ep'), may hold values from -0.375 to 0.375
- dense_gate: float32 [2048], replicated, may hold values from -6 to 6
Outputs:
- mixed: bfloat16 [4096, 2048], P(('ep', 'tp'))
The draws below stay inside these ranges and needn't reach their ends.
Inputs may be any that keep to these rules, and one draw needn't show every extreme that they name: `routes`: each row names 2 different experts. Among the 128 rows of one device no expert is named more than 22 times; every draw has a device and an expert with exactly 22.
All inputs are finite; a program needn't handle non-finite values.
Results may differ from the reference program's by a relative error of at most 0.0074.
Values may be sent and summed in bfloat16 or wider, within the bound.
A program may use at most 128 MiB of HBM per device.

```python
import math
import jax
import jax.numpy as jnp
import numpy as np
from jax import lax

D = 2048
FF = 1024
DH = 256
TOP_K = 2
TOK_DEV = 128
EXPERTS = 16
TOKENS = 4096
CAP = 22
N_TP = 2


def draw_norm_gain(key, part):
    return 1.0 + 0.18 * jnp.clip(jax.random.normal(key, (D,), jnp.float32), -4.0, 4.0)


def shard_levels(key, shape, pieces, low, largest):
    factor_of = 1.0
    for axis_at, blocks in pieces:
        steps = jax.random.uniform(jax.random.fold_in(jax.random.fold_in(key, 6), axis_at), (blocks,), jnp.float32, low / len(pieces), largest / len(pieces))
        factor_of = factor_of * jnp.repeat(jnp.exp(steps), shape[axis_at] // blocks).reshape((-1,) + (1,) * (len(shape) - 1 - axis_at))
    return factor_of


def assign_block(own_key, own, number, rows, amount, top, bound, slope):
    order = jax.random.permutation(own_key, amount)
    packed, common = portions_of(amount, rows * top, bound, slope, True), portions_of(amount, rows * top, bound, slope, False)
    places = jnp.arange(amount)

    def named(lengths, turn):
        used = int((lengths > 0).sum())
        fixed = max(1, used // 4)
        passed = fixed + (places - fixed + turn * (used - fixed)) % max(1, amount - fixed)
        return jnp.zeros((amount,), jnp.int32).at[order[jnp.where(places < fixed, places, passed)]].set(jnp.asarray(lengths, jnp.int32))

    lengths = jnp.where(number % 4 == 0, named(packed, number // 4), named(common, number - number // 4 - 1))
    mixed = jax.random.permutation(jax.random.fold_in(own, 3), amount)
    donor, sink = mixed[0:amount // 2 * 2:2], mixed[1:amount // 2 * 2:2]
    margin = jnp.minimum(lengths[donor] - 1, bound - lengths[sink]) // 2
    margin = jnp.where((donor == order[0]) | (sink == order[0]) | (lengths[sink] == 0), 0, jnp.maximum(margin, 0))
    passed = jax.random.randint(jax.random.fold_in(own, 4), (amount // 2,), 0, 1 << 20) % (margin + 1)
    lengths = lengths.at[donor].add(-passed).at[sink].add(passed)
    items = jnp.searchsorted(jnp.cumsum(lengths), jnp.arange(rows * top), side="right").astype(jnp.int32)
    table = items.reshape(top, rows).T
    table = table[jax.random.permutation(jax.random.fold_in(own, 1), rows)]
    turn = jax.random.randint(jax.random.fold_in(own, 2), (rows, 1), 0, top)
    return jnp.take_along_axis(table, (jnp.arange(top)[None, :] + turn) % top, axis=1)


def portions_of(amount, total, reach, skew, full):
    loads = [(1 << 20) // math.isqrt(standing ** skew) + 1 for standing in range(1, amount + 1)]
    largest = reach if full else min(reach, max(-(-total // amount), total * loads[0] // sum(loads)))
    least = 1 if total - largest >= amount - 1 else 0
    given, spare = [largest] + [least] * (amount - 1), total - largest - least * (amount - 1)
    while spare > 0:
        free = [i for i in range(1, amount) if given[i] < largest] or [i for i in range(1, amount) if given[i] < reach]
        mass, left = sum([loads[i] for i in free]), spare
        for i in free:
            addition = min(reach - given[i], max(1, left * loads[i] // mass), spare)
            given[i] = given[i] + addition
            spare = spare - addition
    return np.array(given)


def noise(rng, dims, width, reach, split=(), kind=jnp.bfloat16):
    array = jax.random.normal(rng, dims, jnp.float32) * width
    if len(split) > 0:
        array = shard_levels(rng, dims, split, -0.22, 0.18) * array
    return jnp.clip(array, min=-reach, max=reach).astype(kind)


def setup_inputs(seed: int = 0) -> dict:
    key_of = jax.random.split(jax.random.key(seed), 11)
    tokens = noise(key_of[0], (TOKENS, D), 1.0, 6.0, ((0, 32),))
    norm_gain = draw_norm_gain(jax.random.fold_in(key_of[10], 71), 0)
    routes_keys = jax.random.split(jax.random.fold_in(key_of[2], 1), TOKENS // TOK_DEV)
    routes_turns = jax.random.permutation(jax.random.fold_in(key_of[2], 3), TOKENS // TOK_DEV)
    routes = jax.vmap(lambda own, number: assign_block(jax.random.fold_in(key_of[2], 2), own, number, TOK_DEV, EXPERTS, TOP_K, CAP, 2))(routes_keys, routes_turns).reshape((TOKENS, TOP_K))
    route_weights = jnp.clip(0.1 + 0.9 * jax.random.uniform(key_of[3], (TOKENS, TOP_K), jnp.float32) ** shard_levels(key_of[3], (TOKENS, TOP_K), ((0, 32),), -0.2, 0.2), 0.1, 1.0)
    w_gate = noise(key_of[4], (EXPERTS, D, FF), D ** -0.5, 0.125, ((0, 16), (2, 2)))
    w_up = noise(key_of[5], (EXPERTS, D, FF), D ** -0.5, 0.125, ((0, 16), (2, 2)))
    w_down = noise(key_of[6], (EXPERTS, FF, D), FF ** -0.5, 0.1875, ((0, 16), (1, 2)))
    dense_in = noise(key_of[7], (D, DH), D ** -0.5, 0.125, ((0, 16),))
    dense_out = noise(key_of[8], (D, DH), DH ** -0.5, 0.375, ((0, 16),))
    dense_gate = noise(key_of[9], (D,), 1.5, 6.0, (), jnp.float32)
    return dict(tokens=tokens, norm_gain=norm_gain, routes=routes, route_weights=route_weights, w_gate=w_gate, w_up=w_up, w_down=w_down, dense_in=dense_in, dense_out=dense_out, dense_gate=dense_gate)


CLAMP_LIMIT = 7.0
SLOPE_ALPHA = 1.702
NORM_EPS = 1e-06

def rms_normed(tokens, norm_gain):
    widened = tokens.astype(jnp.float32)
    inv_scale = lax.rsqrt(lax.optimization_barrier(jnp.mean(widened * widened, axis=1, keepdims=True)) + NORM_EPS)
    return (widened * inv_scale * norm_gain).astype(jnp.bfloat16)

def clamped_unit(gate_pre, up_pre):
    gate_clip = jnp.minimum(gate_pre, CLAMP_LIMIT)
    up_clip = jnp.clip(up_pre, -CLAMP_LIMIT, CLAMP_LIMIT)
    return ((up_clip + 1.0) * gate_clip * jax.nn.sigmoid(SLOPE_ALPHA * gate_clip)).astype(jnp.bfloat16)

def reference(tokens, norm_gain, routes, route_weights, w_gate, w_up, w_down, dense_in, dense_out, dense_gate):
    normed = rms_normed(tokens, norm_gain)
    sources = TOKENS // TOK_DEV
    entries = TOK_DEV * TOP_K
    block_routes = routes.reshape(sources, entries)
    onehot = (block_routes[:, :, None] == jnp.arange(EXPERTS, dtype=jnp.int32)[None, None, :]).astype(jnp.int32)
    slot_index = lax.optimization_barrier(jnp.sum((jnp.cumsum(onehot, axis=1) - onehot) * onehot, axis=2))
    source_ids = jnp.arange(sources, dtype=jnp.int32)[:, None]
    position = (block_routes * (sources * CAP) + source_ids * CAP + slot_index).reshape(-1).astype(jnp.int32)
    entry_ids = jnp.arange(TOKENS * TOP_K, dtype=jnp.int32)
    slot_table = jnp.full((EXPERTS * sources * CAP,), -1, jnp.int32).at[position].set(entry_ids)
    slot_table = slot_table.reshape(EXPERTS, sources * CAP)
    half_width = FF // N_TP

    def one_expert(expert_args):
        entry_index, gate_w, up_w, down_w = expert_args
        is_valid = entry_index >= 0
        token_of = jnp.where(is_valid, entry_index, 0) // TOP_K
        gathered_rows = jnp.where(is_valid[:, None], normed[token_of], jnp.zeros((), jnp.bfloat16))
        gate_pre = jnp.dot(gathered_rows, gate_w, preferred_element_type=jnp.float32)
        up_pre = jnp.dot(gathered_rows, up_w, preferred_element_type=jnp.float32)
        hidden = clamped_unit(gate_pre, up_pre)
        summed = jnp.zeros((gathered_rows.shape[0], D), jnp.float32)
        for half_index in range(N_TP):
            low = half_index * half_width
            partial_value = jnp.dot(hidden[:, low:low + half_width], down_w[low:low + half_width], preferred_element_type=jnp.float32).astype(jnp.bfloat16)
            summed = summed + lax.optimization_barrier(partial_value).astype(jnp.float32)
        return summed.astype(jnp.bfloat16)
    results = lax.map(one_expert, (slot_table, w_gate, w_up, w_down))
    flat_results = results.reshape(EXPERTS * sources * CAP, D)
    picked = flat_results[position].astype(jnp.float32).reshape(TOKENS, TOP_K, D)
    weighted = lax.optimization_barrier(jnp.sum(picked * route_weights[:, :, None], axis=1))
    dense_hidden = jax.nn.silu(jnp.dot(normed, dense_in, preferred_element_type=jnp.float32)).astype(jnp.bfloat16)
    branch = lax.dot_general(dense_hidden, dense_out, (((1,), (1,)), ((), ())), preferred_element_type=jnp.float32)
    return (weighted + jax.nn.sigmoid(dense_gate) * branch).astype(jnp.bfloat16)
```

```python
import functools

import jax
import jax.numpy as jnp
from jax import lax
from jax.experimental import pallas as pl
from jax.experimental.pallas import tpu as pltpu
from jax.sharding import PartitionSpec as P

CLAMP_LIMIT = 7.0
SLOPE_ALPHA = 1.702
NORM_EPS = 1e-06
MESH = pl.DeviceIdType.MESH
F32 = jnp.float32
BF16 = jnp.bfloat16


def clamped_unit(gate_pre, up_pre):
    gate_clip = jnp.minimum(gate_pre, CLAMP_LIMIT)
    up_clip = jnp.clip(up_pre, -CLAMP_LIMIT, CLAMP_LIMIT)
    return ((up_clip + 1.0) * gate_clip * jax.nn.sigmoid(SLOPE_ALPHA * gate_clip)).astype(BF16)


def layer_kernel(
    sizes,
    routes_ref,
    weights_ref,
    tokens_ref,
    gain_ref,
    dgate_ref,
    din_ref,
    dout_ref,
    wg_ref,
    wu_ref,
    wd_ref,
    out_ref,
    normed,
    slots,
    buf,
    recv,
    outb,
    ret,
    wgs,
    wus,
    wds,
    hid,
    dn,
    acc,
    send1,
    recv1,
    send2,
    recv2,
    w_local,
    w_send,
    w_recv,
    ds1,
    dr1,
    ds2,
    dr2,
    ds3,
    dr3,
):
    n, n1, n2, cap = sizes
    rows, width = tokens_ref.shape
    half = wg_ref.shape[1]
    me = lax.axis_index("ep")
    core = lax.axis_index("tp")
    plane, spot = me // n2, me % n2
    peer = 1 - core

    barrier = pltpu.get_barrier_semaphore()

    def greet(i, carry):
        pl.semaphore_signal(
            barrier, inc=1, device_id={"ep": (me + i) % n}, device_id_type=MESH
        )
        return carry

    lax.fori_loop(1, n, greet, 0)
    pl.semaphore_signal(barrier, inc=1, device_id={"tp": peer}, device_id_type=MESH)

    weight_pairs = ((wg_ref, wgs), (wu_ref, wus), (wd_ref, wds))
    for i, (src, dst) in enumerate(weight_pairs):
        pltpu.make_async_copy(src, dst.at[0], w_local.at[i]).start()

    @pl.when(core == 0)
    def _():
        dn[0, plane, spot] = din_ref[...]

    @pl.when(core == 1)
    def _():
        dn[1, plane, spot] = dout_ref[...]

    widened = tokens_ref[...].astype(F32)
    inv_scale = lax.rsqrt(jnp.mean(widened * widened, axis=1, keepdims=True) + NORM_EPS)
    normed[...] = (widened * inv_scale * gain_ref[...]).astype(BF16)

    expert_ids = lax.broadcasted_iota(jnp.int32, (n, rows), 0)
    chosen = (routes_ref[0:1, :] == expert_ids) | (routes_ref[1:2, :] == expert_ids)
    earlier = (
        lax.broadcasted_iota(jnp.int32, (rows, rows), 0)
        < lax.broadcasted_iota(jnp.int32, (rows, rows), 1)
    )
    counted = jnp.dot(
        jnp.where(chosen, 1.0, 0.0).astype(BF16),
        jnp.where(earlier, 1.0, 0.0).astype(BF16),
        preferred_element_type=F32,
    )
    slots[...] = jnp.where(chosen, counted.astype(jnp.int32), -1)

    pl.semaphore_wait(barrier, n)

    def weight_copy(i):
        src, dst = weight_pairs[i]
        return pltpu.make_async_remote_copy(
            src_ref=src,
            dst_ref=dst.at[1],
            send_sem=w_send.at[i],
            recv_sem=w_recv.at[i],
            device_id={"tp": peer},
            device_id_type=MESH,
        )

    def dense_copy1(other):
        return pltpu.make_async_remote_copy(
            src_ref=dn.at[core, plane, spot],
            dst_ref=dn.at[core, plane, spot],
            send_sem=ds1.at[other],
            recv_sem=dr1.at[plane],
            device_id={"ep": other * n2 + spot},
            device_id_type=MESH,
        )

    def dense_wait1(other):
        pltpu.make_async_remote_copy(
            src_ref=dn.at[core, other, spot],
            dst_ref=dn.at[core, other, spot],
            send_sem=ds1.at[other],
            recv_sem=dr1.at[other],
            device_id={"ep": other * n2 + spot},
            device_id_type=MESH,
        ).wait_recv()

    def dense_copy2(other, slot):
        return pltpu.make_async_remote_copy(
            src_ref=dn.at[core, :, slot],
            dst_ref=dn.at[core, :, slot],
            send_sem=ds2.at[other],
            recv_sem=dr2.at[slot],
            device_id={"ep": plane * n2 + other},
            device_id_type=MESH,
        )

    def dense_copy3(which):
        return pltpu.make_async_remote_copy(
            src_ref=dn.at[which],
            dst_ref=dn.at[which],
            send_sem=ds3,
            recv_sem=dr3,
            device_id={"tp": peer},
            device_id_type=MESH,
        )

    def each(count, act):
        def step(i, carry):
            act(i)
            return carry

        lax.fori_loop(0, count, step, 0)

    each(n1 - 1, lambda i: dense_copy1((plane + 1 + i) % n1).start())
    for i in range(3):
        weight_copy(i).start()

    def dispatch(dst, slot):
        return pltpu.make_async_remote_copy(
            src_ref=buf.at[dst],
            dst_ref=recv.at[slot],
            send_sem=send1.at[dst],
            recv_sem=recv1.at[slot],
            device_id={"ep": dst},
            device_id_type=MESH,
        )

    def give_back(dst, slot):
        return pltpu.make_async_remote_copy(
            src_ref=outb.at[dst],
            dst_ref=ret.at[slot],
            send_sem=send2.at[dst],
            recv_sem=recv2.at[slot],
            device_id={"ep": dst},
            device_id_type=MESH,
        )

    def shift_of(i):
        later = (n1 // 2 + i - 2) % (n1 - 1) + 1
        return jnp.where(i == 0, 0, later)

    tile = min(512, width)

    def send_group(i):
        group = (plane + shift_of((i + 1) % n1)) % n1
        first = group * n2
        wanted = slots[pl.ds(first, n2), :]
        picks = wanted[:, None, :] == lax.broadcasted_iota(jnp.int32, (n2, cap, rows), 1)
        picks = jnp.where(picks, 1.0, 0.0).reshape(n2 * cap, rows).astype(BF16)
        for low in range(0, width, tile):
            found = jnp.dot(picks, normed[:, low : low + tile], preferred_element_type=F32)
            buf[pl.ds(first, n2), :, low : low + tile] = found.reshape(n2, cap, tile).astype(BF16)

        def start(j):
            dst = first + (spot + 1 + j) % n2

            @pl.when(dst != me)
            def _():
                dispatch(dst, me).start()

            @pl.when(dst == me)
            def _():
                recv[me] = buf[me]

        each(n2, start)

    each(n1, send_group)

    each(n1 - 1, lambda i: dense_wait1((plane + 1 + i) % n1))
    each(n2 - 1, lambda i: dense_copy2((spot + 1 + i) % n2, spot).start())

    for i, (src, dst) in enumerate(weight_pairs):
        pltpu.make_async_copy(src, dst.at[0], w_local.at[i]).wait()
    for i in range(3):
        weight_copy(i).wait()

    piece = min(256, half)

    def run_group(i):
        group = (plane - shift_of(i) + n1) % n1
        first = group * n2

        def arrive(j):
            src = first + j

            @pl.when(src != me)
            def _():
                dispatch(src, src).wait_recv()

        each(n2, arrive)
        x = recv[pl.ds(first, n2)].astype(F32).reshape(n2 * cap, width).astype(BF16)
        for part in range(2):
            for low in range(0, half, piece):
                gate_pre = jnp.dot(
                    x, wgs[part, :, low : low + piece], preferred_element_type=F32
                )
                up_pre = jnp.dot(x, wus[part, :, low : low + piece], preferred_element_type=F32)
                hid[part, :, low : low + piece] = clamped_unit(gate_pre, up_pre)
        for low in range(0, width, tile):
            total = jnp.zeros((n2 * cap, tile), F32)
            for part in range(2):
                partial = jnp.dot(
                    hid[part], wds[part, :, low : low + tile], preferred_element_type=F32
                )
                total = total + partial.astype(BF16).astype(F32)
            outb[pl.ds(first, n2), :, low : low + tile] = total.reshape(n2, cap, tile).astype(BF16)

        def start(j):
            dst = first + (spot + 1 + j) % n2

            @pl.when(dst != me)
            def _():
                give_back(dst, me).start()

            @pl.when(dst == me)
            def _():
                ret[me] = outb[me]

        each(n2, start)

    each(n1 // 2, run_group)
    each(n2 - 1, lambda i: dense_copy2((spot + 1 + i) % n2, (spot + 1 + i) % n2).wait_recv())
    dense_copy3(core).start()
    each(n1 - n1 // 2, lambda i: run_group(i + n1 // 2))

    dense_copy3(core).wait_send()
    dense_copy3(peer).wait_recv()
    depth = din_ref.shape[1]
    dense_pre = jnp.dot(
        normed[...], dn[0].reshape(width, depth), preferred_element_type=F32
    )
    dense_hidden = jax.nn.silu(dense_pre).astype(BF16)
    step = width // n1
    for z in range(n1):
        branch = lax.dot_general(
            dense_hidden,
            dn[1, z].reshape(step, depth),
            (((1,), (1,)), ((), ())),
            preferred_element_type=F32,
        )
        acc[:, z * step : (z + 1) * step] = (
            jax.nn.sigmoid(dgate_ref[:, z * step : (z + 1) * step]) * branch
        )

    def settle(i):
        other = (me + 1 + i) % n
        give_back(other, other).wait_recv()

    each(n - 1, settle)

    places = lax.broadcasted_iota(jnp.int32, (n, cap, rows), 1)
    here = slots[...][:, None, :] == places
    takes = []
    for k in range(2):
        mine = (routes_ref[k : k + 1, :] == expert_ids)[:, None, :]
        take = jnp.where(here & mine, 1.0, 0.0).reshape(n * cap, rows)
        takes.append(take.T.astype(BF16))
    for low in range(0, width, tile):
        back = ret[:, :, low : low + tile].astype(F32).reshape(n * cap, tile).astype(BF16)
        total = acc[:, low : low + tile]
        for k in range(2):
            picked = jnp.dot(takes[k], back, preferred_element_type=F32)
            total = total + picked * weights_ref[:, k : k + 1]
        out_ref[:, low : low + tile] = total.astype(BF16)

    def drain(i):
        other = (me + 1 + i) % n
        dispatch(other, me).wait_send()
        give_back(other, me).wait_send()

    each(n - 1, drain)
    each(n1 - 1, lambda i: dense_copy1((plane + 1 + i) % n1).wait_send())
    each(n2 - 1, lambda i: dense_copy2((spot + 1 + i) % n2, spot).wait_send())


def shards(
    tokens, norm_gain, routes, route_weights, w_gate, w_up, w_down, dense_in, dense_out, dense_gate
):
    rows, width = tokens.shape
    top_count = routes.shape[1]
    n = lax.axis_size("ep")
    capacity = (4 * rows * top_count + 3 * n - 1) // (3 * n)
    cap = -(-capacity // 8) * 8
    n2 = 1
    while n2 * n2 < n:
        n2 *= 2
    n1 = n // n2
    half = w_gate.shape[2]
    depth = dense_in.shape[1]
    vmem = pl.BlockSpec(memory_space=pltpu.VMEM)
    anywhere = pl.BlockSpec(memory_space=pl.ANY)
    dma = pltpu.SemaphoreType.DMA
    slab = pltpu.VMEM((n, cap, width), BF16)
    return pl.pallas_call(
        functools.partial(layer_kernel, (n, n1, n2, cap)),
        out_shape=jax.ShapeDtypeStruct((rows, width), BF16),
        in_specs=[vmem] * 7 + [anywhere] * 3,
        out_specs=vmem,
        scratch_shapes=[
            pltpu.VMEM((rows, width), BF16),
            pltpu.VMEM((n, rows), jnp.int32),
            slab,
            slab,
            slab,
            slab,
            pltpu.VMEM((2, width, half), BF16),
            pltpu.VMEM((2, width, half), BF16),
            pltpu.VMEM((2, half, width), BF16),
            pltpu.VMEM((2, n2 * cap, half), BF16),
            pltpu.VMEM((2, n1, n2, width // n, depth), BF16),
            pltpu.VMEM((rows, width), F32),
            dma((n,)),
            dma((n,)),
            dma((n,)),
            dma((n,)),
            dma((3,)),
            dma((3,)),
            dma((3,)),
            dma((n1,)),
            dma((n1,)),
            dma((n2,)),
            dma((n2,)),
            dma,
            dma,
        ],
        compiler_params=pltpu.CompilerParams(
            collective_id=0, has_side_effects=True, vmem_limit_bytes=60 * 1024 * 1024
        ),
    )(
        routes.T,
        route_weights,
        tokens,
        norm_gain.reshape(1, width),
        dense_gate.reshape(1, width),
        dense_in,
        dense_out,
        w_gate[0],
        w_up[0],
        w_down[0],
    )


def solution(mesh):
    placed = (
        P(("ep", "tp"), None),
        P(),
        P(("ep", "tp"), None),
        P(("ep", "tp"), None),
        P("ep", None, "tp"),
        P("ep", None, "tp"),
        P("ep", "tp", None),
        P("ep", None),
        P("ep", None),
        P(),
    )
    return jax.shard_map(
        shards, mesh=mesh, in_specs=placed, out_specs=P(("ep", "tp"), None), check_vma=False
    )
```

```python
import functools
import math

import jax
import jax.numpy as jnp
from jax import lax
from jax.experimental import pallas as pl
from jax.experimental.pallas import tpu as pltpu
from jax.sharding import PartitionSpec as P

CLAMP_LIMIT = 7.0
SLOPE_ALPHA = 1.702
NORM_EPS = 1e-06
MESH = pl.DeviceIdType.MESH
F32 = jnp.float32
BF16 = jnp.bfloat16


def clamped_unit(gate_pre, up_pre):
    gate_clip = jnp.minimum(gate_pre, CLAMP_LIMIT)
    up_clip = jnp.clip(up_pre, -CLAMP_LIMIT, CLAMP_LIMIT)
    return ((up_clip + 1.0) * gate_clip * jax.nn.sigmoid(SLOPE_ALPHA * gate_clip)).astype(BF16)


def layer_kernel(
    sizes,
    routes_t_ref,
    routes_ref,
    weights_ref,
    tokens_ref,
    gain_ref,
    dgate_ref,
    din_ref,
    dout_ref,
    wg_ref,
    wu_ref,
    wd_ref,
    out_ref,
    normed,
    keys,
    stacked,
    places,
    xs,
    totals,
    unpack_ref,
    pack_ref,
    buf,
    recv,
    outb,
    ret,
    wgs,
    wus,
    wds,
    hid,
    dn,
    acc,
    send1,
    recv1,
    send2,
    recv2,
    w_local,
    w_send,
    w_recv,
    ds1,
    dr1,
    ds2,
    dr2,
    ds3,
    dr3,
):
    n, n1, n2, cap, blocks = sizes
    rows, width = tokens_ref.shape
    half = wg_ref.shape[1]
    tall, tile = blocks * cap, width // blocks
    group_rows, packed_rows = n2 * cap, n2 * blocks * cap
    me = lax.axis_index("ep")
    core = lax.axis_index("tp")
    plane, spot = me // n2, me % n2
    peer = 1 - core

    barrier = pltpu.get_barrier_semaphore()

    def greet(i, carry):
        pl.semaphore_signal(
            barrier, inc=1, device_id={"ep": (me + i) % n}, device_id_type=MESH
        )
        return carry

    lax.fori_loop(1, n, greet, 0)
    pl.semaphore_signal(barrier, inc=1, device_id={"tp": peer}, device_id_type=MESH)

    weight_pairs = ((wg_ref, wgs), (wu_ref, wus), (wd_ref, wds))
    for i, (src, dst) in enumerate(weight_pairs):
        pltpu.make_async_copy(src, dst.at[0], w_local.at[i]).start()

    @pl.when(core == 0)
    def _():
        dn[0, plane, spot] = din_ref[...]

    @pl.when(core == 1)
    def _():
        dn[1, plane, spot] = dout_ref[...]

    widened = tokens_ref[...].astype(F32)
    inv_scale = lax.rsqrt(jnp.mean(widened * widened, axis=1, keepdims=True) + NORM_EPS)
    normed[...] = (widened * inv_scale * gain_ref[...]).astype(BF16)
    for j in range(blocks):
        stacked[j * rows : (j + 1) * rows, :] = normed[:, j * tile : (j + 1) * tile]

    expert_ids = lax.broadcasted_iota(jnp.int32, (n, rows), 0)
    chosen = (routes_t_ref[0:1, :] == expert_ids) | (routes_t_ref[1:2, :] == expert_ids)
    earlier = (
        lax.broadcasted_iota(jnp.int32, (rows, rows), 0)
        < lax.broadcasted_iota(jnp.int32, (rows, rows), 1)
    )
    counted = jnp.dot(
        jnp.where(chosen, 1.0, 0.0).astype(BF16),
        jnp.where(earlier, 1.0, 0.0).astype(BF16),
        preferred_element_type=F32,
    )
    for j in range(blocks):
        found = jnp.where(chosen, counted.astype(jnp.int32) + j * cap, -1)
        for z in range(n1):
            keys[z, :, j * rows : (j + 1) * rows] = found[z * n2 : (z + 1) * n2]
    experts_across = lax.broadcasted_iota(jnp.int32, (rows, n), 1)
    takes = [routes_ref[:, k : k + 1] == experts_across for k in range(2)]
    before = (
        lax.broadcasted_iota(jnp.int32, (rows, rows), 0)
        > lax.broadcasted_iota(jnp.int32, (rows, rows), 1)
    )
    counts = jnp.dot(
        jnp.where(before, 1.0, 0.0).astype(BF16),
        jnp.where(takes[0] | takes[1], 1.0, 0.0).astype(BF16),
        preferred_element_type=F32,
    )
    for k in range(2):
        slot = jnp.sum(jnp.where(takes[k], counts, 0.0), axis=1, keepdims=True)
        places[:, k : k + 1] = routes_ref[:, k : k + 1] * tall + slot.astype(jnp.int32)

    pl.semaphore_wait(barrier, n)

    def weight_copy(i):
        src, dst = weight_pairs[i]
        return pltpu.make_async_remote_copy(
            src_ref=src,
            dst_ref=dst.at[1],
            send_sem=w_send.at[i],
            recv_sem=w_recv.at[i],
            device_id={"tp": peer},
            device_id_type=MESH,
        )

    def dense_copy1(bit, block):
        other = plane + bit - 2 * bit * ((plane // bit) % 2)
        return pltpu.make_async_remote_copy(
            src_ref=dn.at[core, block, spot],
            dst_ref=dn.at[core, block, spot],
            send_sem=ds1.at[block],
            recv_sem=dr1.at[block],
            device_id={"ep": other * n2 + spot},
            device_id_type=MESH,
        )

    bits = [1 << b for b in reversed(range(n1.bit_length() - 1))]

    def dense_held(bit, where):
        return [where % (2 * bit) + m * 2 * bit for m in range(n1 // (2 * bit))]

    def dense_start(bit):
        for block in dense_held(bit, plane):
            dense_copy1(bit, block).start()

    def dense_finish(bit):
        for block in dense_held(bit, plane + bit - 2 * bit * ((plane // bit) % 2)):
            dense_copy1(bit, block).wait_recv()
        for block in dense_held(bit, plane):
            dense_copy1(bit, block).wait_send()

    def dense_copy2(other, slot):
        return pltpu.make_async_remote_copy(
            src_ref=dn.at[core, :, slot],
            dst_ref=dn.at[core, :, slot],
            send_sem=ds2.at[other],
            recv_sem=dr2.at[slot],
            device_id={"ep": plane * n2 + other},
            device_id_type=MESH,
        )

    def dense_copy3(which):
        return pltpu.make_async_remote_copy(
            src_ref=dn.at[which],
            dst_ref=dn.at[which],
            send_sem=ds3,
            recv_sem=dr3,
            device_id={"tp": peer},
            device_id_type=MESH,
        )

    def each(count, act):
        def step(i, carry):
            act(i)
            return carry

        lax.fori_loop(0, count, step, 0)

    dense_start(bits[0])
    for i in range(3):
        weight_copy(i).start()

    def dispatch(dst, slot):
        return pltpu.make_async_remote_copy(
            src_ref=buf.at[dst],
            dst_ref=recv.at[slot],
            send_sem=send1.at[dst],
            recv_sem=recv1.at[slot],
            device_id={"ep": dst},
            device_id_type=MESH,
        )

    def give_back(dst, slot):
        return pltpu.make_async_remote_copy(
            src_ref=outb.at[dst],
            dst_ref=ret.at[slot],
            send_sem=send2.at[dst],
            recv_sem=recv2.at[slot],
            device_id={"ep": dst},
            device_id_type=MESH,
        )

    def shift_of(i):
        later = (n1 // 2 + i - 2) % (n1 - 1) + 1
        return jnp.where(i == 0, 0, later)

    def send_group(i):
        group = (plane + shift_of((i + 1) % n1)) % n1
        first = group * n2
        wanted = keys[group]
        picks = wanted[:, None, :] == lax.broadcasted_iota(
            jnp.int32, (n2, tall, blocks * rows), 1
        )
        picks = jnp.where(picks, 1.0, 0.0).reshape(packed_rows, blocks * rows).astype(BF16)
        found = jnp.dot(picks, stacked[...], preferred_element_type=F32)
        buf[pl.ds(first, n2)] = found.reshape(n2, tall, tile).astype(BF16)

        def start(j):
            dst = first + (spot + 1 + j) % n2

            @pl.when(dst != me)
            def _():
                dispatch(dst, me).start()

            @pl.when(dst == me)
            def _():
                recv[me] = buf[me]

        each(n2, start)

    each(n1, send_group)

    for bit, following in zip(bits, bits[1:] + [None]):
        dense_finish(bit)
        if following is not None:
            dense_start(following)
    each(n2 - 1, lambda i: dense_copy2((spot + 1 + i) % n2, spot).start())

    for i, (src, dst) in enumerate(weight_pairs):
        pltpu.make_async_copy(src, dst.at[0], w_local.at[i]).wait()
    for i in range(3):
        weight_copy(i).wait()

    piece = min(256, half)
    upright = lax.broadcasted_iota(jnp.int32, (packed_rows, packed_rows), 0)
    across = lax.broadcasted_iota(jnp.int32, (packed_rows, packed_rows), 1)

    def packed_place(r):
        return (r // cap) % n2 * tall + r // group_rows * cap + r % cap

    unpack = jnp.where(packed_place(upright) == across, 1.0, 0.0).astype(BF16)
    pack = jnp.where(packed_place(across) == upright, 1.0, 0.0).astype(BF16)
    unpack_ref[...] = unpack
    pack_ref[...] = pack

    def run_group(i):
        group = (plane - shift_of(i) + n1) % n1
        first = group * n2

        def arrive(j):
            src = first + j

            @pl.when(src != me)
            def _():
                dispatch(src, src).wait_recv()

        each(n2, arrive)
        came = recv[pl.ds(first, n2)].astype(F32).reshape(packed_rows, tile).astype(BF16)
        apart = jnp.dot(unpack_ref[...], came, preferred_element_type=F32)
        for j in range(blocks):
            xs[:, j * tile : (j + 1) * tile] = apart[
                j * group_rows : (j + 1) * group_rows
            ].astype(BF16)
        x = xs[...]
        for part in range(2):
            for low in range(0, half, piece):
                gate_pre = jnp.dot(
                    x, wgs[part, :, low : low + piece], preferred_element_type=F32
                )
                up_pre = jnp.dot(x, wus[part, :, low : low + piece], preferred_element_type=F32)
                hid[part, :, low : low + piece] = clamped_unit(gate_pre, up_pre)
        for j in range(blocks):
            total = jnp.zeros((group_rows, tile), F32)
            for part in range(2):
                partial = jnp.dot(
                    hid[part],
                    wds[part, :, j * tile : (j + 1) * tile],
                    preferred_element_type=F32,
                )
                total = total + partial.astype(BF16).astype(F32)
            totals[j * group_rows : (j + 1) * group_rows, :] = total
        joined = jnp.dot(pack_ref[...], totals[...].astype(BF16), preferred_element_type=F32)
        outb[pl.ds(first, n2)] = joined.reshape(n2, tall, tile).astype(BF16)

        def start(j):
            dst = first + (spot + 1 + j) % n2

            @pl.when(dst != me)
            def _():
                give_back(dst, me).start()

            @pl.when(dst == me)
            def _():
                ret[me] = outb[me]

        each(n2, start)

    each(n1 // 2, run_group)
    each(n2 - 1, lambda i: dense_copy2((spot + 1 + i) % n2, (spot + 1 + i) % n2).wait_recv())
    dense_copy3(core).start()
    each(n1 - n1 // 2, lambda i: run_group(i + n1 // 2))

    dense_copy3(core).wait_send()
    dense_copy3(peer).wait_recv()
    depth = din_ref.shape[1]
    dense_pre = jnp.dot(
        normed[...], dn[0].reshape(width, depth), preferred_element_type=F32
    )
    dense_hidden = jax.nn.silu(dense_pre).astype(BF16)
    step = width // n1
    for z in range(n1):
        branch = lax.dot_general(
            dense_hidden,
            dn[1, z].reshape(step, depth),
            (((1,), (1,)), ((), ())),
            preferred_element_type=F32,
        )
        acc[:, z * step : (z + 1) * step] = (
            jax.nn.sigmoid(dgate_ref[:, z * step : (z + 1) * step]) * branch
        )

    def combine_group(i):
        group = (plane + shift_of(i)) % n1
        first = group * n2

        def arrive(j):
            src = first + j

            @pl.when(src != me)
            def _():
                give_back(src, src).wait_recv()

        each(n2, arrive)
        back = ret[pl.ds(first, n2)].astype(F32).reshape(packed_rows, tile).astype(BF16)
        lanes = lax.broadcasted_iota(jnp.int32, (rows, packed_rows), 1) + first * tall
        wanted = jnp.concatenate(
            [
                jnp.where(places[:, k : k + 1] + j * cap == lanes, 1.0, 0.0).astype(BF16)
                for k in range(2)
                for j in range(blocks)
            ],
            axis=0,
        )
        picked = jnp.dot(wanted, back, preferred_element_type=F32)
        for j in range(blocks):
            total = acc[:, j * tile : (j + 1) * tile]
            for k in range(2):
                at = (k * blocks + j) * rows
                total = total + picked[at : at + rows] * weights_ref[:, k : k + 1]
            acc[:, j * tile : (j + 1) * tile] = total

    each(n1, combine_group)
    out_ref[...] = acc[...].astype(BF16)

    def drain(i):
        other = (me + 1 + i) % n
        dispatch(other, me).wait_send()
        give_back(other, me).wait_send()

    each(n - 1, drain)
    each(n2 - 1, lambda i: dense_copy2((spot + 1 + i) % n2, spot).wait_send())


def shards(
    tokens, norm_gain, routes, route_weights, w_gate, w_up, w_down, dense_in, dense_out, dense_gate
):
    rows, width = tokens.shape
    top_count = routes.shape[1]
    n = lax.axis_size("ep")
    capacity = (4 * rows * top_count + 3 * n - 1) // (3 * n)
    cap = capacity
    blocks = 8 // math.gcd(cap, 8)
    tall, tile = blocks * cap, width // blocks
    n2 = 1
    while n2 * n2 < n:
        n2 *= 2
    n1 = n // n2
    half = w_gate.shape[2]
    depth = dense_in.shape[1]
    vmem = pl.BlockSpec(memory_space=pltpu.VMEM)
    anywhere = pl.BlockSpec(memory_space=pl.ANY)
    dma = pltpu.SemaphoreType.DMA
    slab = pltpu.VMEM((n, tall, tile), BF16)
    return pl.pallas_call(
        functools.partial(layer_kernel, (n, n1, n2, cap, blocks)),
        out_shape=jax.ShapeDtypeStruct((rows, width), BF16),
        in_specs=[vmem] * 8 + [anywhere] * 3,
        out_specs=vmem,
        scratch_shapes=[
            pltpu.VMEM((rows, width), BF16),
            pltpu.VMEM((n1, n2, blocks * rows), jnp.int32),
            pltpu.VMEM((blocks * rows, tile), BF16),
            pltpu.VMEM((rows, 2), jnp.int32),
            pltpu.VMEM((n2 * cap, width), BF16),
            pltpu.VMEM((n2 * tall, tile), F32),
            pltpu.VMEM((n2 * tall, n2 * tall), BF16),
            pltpu.VMEM((n2 * tall, n2 * tall), BF16),
            slab,
            slab,
            slab,
            slab,
            pltpu.VMEM((2, width, half), BF16),
            pltpu.VMEM((2, width, half), BF16),
            pltpu.VMEM((2, half, width), BF16),
            pltpu.VMEM((2, n2 * cap, half), BF16),
            pltpu.VMEM((2, n1, n2, width // n, depth), BF16),
            pltpu.VMEM((rows, width), F32),
            dma((n,)),
            dma((n,)),
            dma((n,)),
            dma((n,)),
            dma((3,)),
            dma((3,)),
            dma((3,)),
            dma((n1,)),
            dma((n1,)),
            dma((n2,)),
            dma((n2,)),
            dma,
            dma,
        ],
        compiler_params=pltpu.CompilerParams(
            collective_id=0, has_side_effects=True, vmem_limit_bytes=60 * 1024 * 1024
        ),
    )(
        routes.T,
        routes,
        route_weights,
        tokens,
        norm_gain.reshape(1, width),
        dense_gate.reshape(1, width),
        dense_in,
        dense_out,
        w_gate[0],
        w_up[0],
        w_down[0],
    )


def solution(mesh):
    placed = (
        P(("ep", "tp"), None),
        P(),
        P(("ep", "tp"), None),
        P(("ep", "tp"), None),
        P("ep", None, "tp"),
        P("ep", None, "tp"),
        P("ep", "tp", None),
        P("ep", None),
        P("ep", None),
        P(),
    )
    return jax.shard_map(
        shards, mesh=mesh, in_specs=placed, out_specs=P(("ep", "tp"), None), check_vma=False
    )
```
